32 devices in a mesh: sp: 8 (over z, x), tp: 4 (over y, core).
Axes of the slice: x: 2, y: 2, z: 4, core: 2. Of those that a mesh axis runs over, the one named last changes fastest.
Arguments:
- queries: bfloat16 [512, 16, 192], P('sp', 'tp'), may hold values from -400 to 400
- latents: bfloat16 [512, 512], P('sp'), may hold values from -6 to 6
- rope_keys: bfloat16 [512, 64], P('sp'), may hold values from -9 to 9
- latent_norm_scale: float32 [512], replicated, may hold values from 0.1 to 1.9
- key_value_weight: bfloat16 [512, 16, 256], P(None, 'tp'), may hold values from -0.25 to 0.25
- out_weight: bfloat16 [2048, 2048], P('tp'), may hold values from -1 to 1
- resid: bfloat16 [512, 2048], P('sp'), may hold values from -3 to 3
- ffn_gain: float32 [2048], replicated, may hold values from 0.1 to 1.9
- expert_ids: int32 [512, 2], P('sp'), may hold values from 0 to 7, all different within a row; in each aligned block of 64 rows (0 to 63, 64 to 127, ...) at most 24 rows name the same one
- route_weights: float32 [512, 2], P('sp'), may hold values from 0.1 to 1
- gate_weight: bfloat16 [8, 2048, 4096], P('sp', None, 'tp'), may hold values from -0.125 to 0.125
- up_weight: bfloat16 [8, 2048, 4096], P('sp', None, 'tp'), may hold values from -0.125 to 0.125
- down_weight: bfloat16 [8, 4096, 2048], P('sp', 'tp'), may hold values from -0.09375 to 0.09375
Outputs:
- updated: bfloat16 [512, 2048], P('sp', 'tp')
The draws below stay inside these ranges and needn't reach their ends.
Inputs may be any that keep to these rules, and one draw needn't show every extreme that they name: `expert_ids`: among the rows of one device no expert is named more than 24 times, and in some devices some expert is named exactly 24 times.
All inputs are finite; a program needn't handle non-finite values.
Results may differ from the reference program's by a relative error of at most 0.025.
Values may be sent and summed in bfloat16 or wider, within the bound.
A program may use at most 64 MiB of HBM per device.

```python
import math
import jax
import jax.numpy as jnp
import numpy as np
from jax import lax

D = 2048
HEAD_COUNT = 16
PLAIN_WIDTH = 128
RD = 64
VALUE_WIDTH = 128
LATENT_WIDTH = 512
FF_E = 4096
TOP = 2
TOK_DEV = 64
TOKEN_COUNT = 512
EXPERTS = 8
CAP = 24
N_SP = 8
N_TP = 4


def drawn_base(key):
    keys_all = jnp.clip(jax.random.normal(jax.random.fold_in(key, 101), (TOKEN_COUNT, RD), jnp.float32), -6.0, 6.0)
    return keys_all


def draw_rope_keys(key, part):
    keys_all = drawn_base(key)
    return keys_all.astype(jnp.bfloat16)


def draw_queries(key, part):
    base = jnp.clip(1.5 * jax.random.normal(jax.random.fold_in(key, 103), (TOKEN_COUNT, HEAD_COUNT, PLAIN_WIDTH + RD), jnp.float32), -9.0, 9.0)
    return base.astype(jnp.bfloat16)


def level_of(stream_key, shape, split, least, largest):
    loudness, own = 1.0, jax.random.fold_in(stream_key, 6)
    for position, shards_of in split:
        steps = jnp.exp(jax.random.uniform(jax.random.fold_in(own, position), (shards_of,), jnp.float32, least / len(split), largest / len(split)))
        loudness = loudness * jnp.repeat(steps, shape[position] // shards_of).reshape([-1 if axis == position else 1 for axis in range(len(shape))])
    return loudness


def deal_out(own_key, own, number, rows, amount, top, reach, lean):
    ranking = jax.random.permutation(own_key, amount)
    heavy_load, ordinary = load_shares(amount, rows * top, reach, lean, True), load_shares(amount, rows * top, reach, lean, False)
    places = jnp.arange(amount)

    def named(tallies, turn):
        used = int((tallies > 0).sum())
        fixed = max(1, used // 4)
        moved = fixed + (places - fixed + turn * (used - fixed)) % max(1, amount - fixed)
        return jnp.zeros((amount,), jnp.int32).at[ranking[jnp.where(places < fixed, places, moved)]].set(jnp.asarray(tallies, jnp.int32))

    tallies = jnp.where(number % 4 == 0, named(heavy_load, number // 4), named(ordinary, number - number // 4 - 1))
    mixed = jax.random.permutation(jax.random.fold_in(own, 3), amount)
    source_of, receiver = mixed[0:amount // 2 * 2:2], mixed[1:amount // 2 * 2:2]
    slack = jnp.minimum(tallies[source_of] - 1, reach - tallies[receiver]) // 2
    slack = jnp.where((source_of == ranking[0]) | (receiver == ranking[0]) | (tallies[receiver] == 0), 0, jnp.maximum(slack, 0))
    moved = jax.random.randint(jax.random.fold_in(own, 4), (amount // 2,), 0, 1 << 20) % (slack + 1)
    tallies = tallies.at[source_of].add(-moved).at[receiver].add(moved)
    items = jnp.searchsorted(jnp.cumsum(tallies), jnp.arange(rows * top), side="right").astype(jnp.int32)
    table = items.reshape(top, rows).T
    table = table[jax.random.permutation(jax.random.fold_in(own, 1), rows)]
    turn = jax.random.randint(jax.random.fold_in(own, 2), (rows, 1), 0, top)
    return jnp.take_along_axis(table, (jnp.arange(top)[None, :] + turn) % top, axis=1)


def load_shares(number_of, total, limit, slope, full):
    loads = [(1 << 20) // math.isqrt(grade ** slope) + 1 for grade in range(1, number_of + 1)]
    largest = limit if full else min(limit, max(-(-total // number_of), total * loads[0] // sum(loads)))
    least = 1 if total - largest >= number_of - 1 else 0
    counts, rest = [largest] + [least] * (number_of - 1), total - largest - least * (number_of - 1)
    while rest > 0:
        free = [i for i in range(1, number_of) if counts[i] < largest] or [i for i in range(1, number_of) if counts[i] < limit]
        mass, remaining = sum([loads[i] for i in free]), rest
        for i in free:
            more = min(limit - counts[i], max(1, remaining * loads[i] // mass), rest)
            counts[i] = counts[i] + more
            rest = rest - more
    return np.array(counts)


def scatter_about(rng, shape, deviation, limit, cuts=(), held_as=jnp.bfloat16):
    result = jax.random.normal(rng, shape, jnp.float32) * deviation
    if len(cuts) > 0:
        result = level_of(rng, shape, cuts, -0.22, 0.18) * result
    return jnp.clip(result, min=-limit, max=limit).astype(held_as)


def setup_inputs(seed: int = 0) -> dict:
    keys = jax.random.split(jax.random.key(seed), 14)
    queries = draw_queries(jax.random.fold_in(keys[13], 71), 0)
    latents = scatter_about(keys[1], (TOKEN_COUNT, LATENT_WIDTH), 1.0, 6.0, ((0, 8),))
    rope_keys = draw_rope_keys(jax.random.fold_in(keys[13], 71), 0)
    latent_norm_scale = jnp.clip(1.0 + 0.18 * jax.random.normal(keys[3], (LATENT_WIDTH,), jnp.float32), 0.1, 1.9)
    key_value_weight = scatter_about(keys[4], (LATENT_WIDTH, HEAD_COUNT, PLAIN_WIDTH + VALUE_WIDTH), LATENT_WIDTH ** -0.5, 0.25, ((1, 4),))
    out_weight = scatter_about(keys[5], (HEAD_COUNT * VALUE_WIDTH, D), (HEAD_COUNT * VALUE_WIDTH // 64) ** -0.5, 1.0, ((0, 4),))
    resid = scatter_about(keys[6], (TOKEN_COUNT, D), 0.5, 3.0, ((0, 8),))
    ffn_gain = jnp.clip(1.0 + 0.18 * jax.random.normal(keys[7], (D,), jnp.float32), 0.1, 1.9)
    expert_ids_keys = jax.random.split(jax.random.fold_in(keys[8], 1), TOKEN_COUNT // TOK_DEV)
    expert_ids_turns = jax.random.permutation(jax.random.fold_in(keys[8], 3), TOKEN_COUNT // TOK_DEV)
    expert_ids = jax.vmap(lambda own, number: deal_out(jax.random.fold_in(keys[8], 2), own, number, TOK_DEV, EXPERTS, TOP, CAP, 2))(expert_ids_keys, expert_ids_turns).reshape((TOKEN_COUNT, TOP))
    route_weights = jnp.clip(0.1 + 0.9 * jax.random.uniform(keys[9], (TOKEN_COUNT, TOP), jnp.float32) ** level_of(keys[9], (TOKEN_COUNT, TOP), ((0, 8),), -0.2, 0.2), 0.1, 1.0)
    gate_weight = scatter_about(keys[10], (EXPERTS, D, FF_E), D ** -0.5, 0.125, ((0, 8), (2, 4)))
    up_weight = scatter_about(keys[11], (EXPERTS, D, FF_E), D ** -0.5, 0.125, ((0, 8), (2, 4)))
    down_weight = scatter_about(keys[12], (EXPERTS, FF_E, D), FF_E ** -0.5, 0.09375, ((0, 8), (1, 4)))
    return {"queries": queries, "latents": latents, "rope_keys": rope_keys, "latent_norm_scale": latent_norm_scale, "key_value_weight": key_value_weight, "out_weight": out_weight, "resid": resid, "ffn_gain": ffn_gain, "expert_ids": expert_ids, "route_weights": route_weights, "gate_weight": gate_weight, "up_weight": up_weight, "down_weight": down_weight}


rope_base = 10000.0
norm_eps = 1e-06

def rotary_table(positions, width):
    half_width = width // 2
    inverse = rope_base ** (-jnp.arange(half_width, dtype=jnp.float32) / half_width)
    turned = positions[:, None] * inverse[None, :]
    return (jnp.cos(turned), jnp.sin(turned))

def turn_pairs(vectors, cosines, sines):
    half_width = vectors.shape[-1] // 2
    front_half = vectors[..., :half_width]
    back_half = vectors[..., half_width:]
    return jnp.concatenate([front_half * cosines - back_half * sines, back_half * cosines + front_half * sines], axis=-1)

def rms_scaled(matrix, gain):
    floats = matrix.astype(jnp.float32)
    return floats * lax.rsqrt(lax.optimization_barrier(jnp.mean(floats * floats, axis=-1, keepdims=True)) + norm_eps) * gain

def reference(queries, latents, rope_keys, latent_norm_scale, key_value_weight, out_weight, resid, ffn_gain, expert_ids, route_weights, gate_weight, up_weight, down_weight):
    positions = jnp.arange(TOKEN_COUNT, dtype=jnp.float32)
    cosines, sines = rotary_table(positions, RD)
    normalized_latent = rms_scaled(latents, latent_norm_scale).astype(jnp.bfloat16)
    projected_rows = jnp.dot(normalized_latent, key_value_weight.reshape(LATENT_WIDTH, HEAD_COUNT * (PLAIN_WIDTH + VALUE_WIDTH)), preferred_element_type=jnp.float32)
    projected_rows = lax.optimization_barrier(projected_rows.astype(jnp.bfloat16)).astype(jnp.float32).reshape(TOKEN_COUNT, HEAD_COUNT, PLAIN_WIDTH + VALUE_WIDTH)
    key_plain = projected_rows[:, :, :PLAIN_WIDTH]
    head_values = projected_rows[:, :, PLAIN_WIDTH:]
    key_turned = turn_pairs(rope_keys.astype(jnp.float32), cosines, sines)
    key_turned = lax.optimization_barrier(key_turned.astype(jnp.bfloat16)).astype(jnp.float32)
    query_plain = queries[:, :, :PLAIN_WIDTH].astype(jnp.float32)
    query_turned = turn_pairs(queries[:, :, PLAIN_WIDTH:].astype(jnp.float32), cosines[:, None, :], sines[:, None, :])
    query_turned = lax.optimization_barrier(query_turned.astype(jnp.bfloat16)).astype(jnp.float32)
    score_scale = (PLAIN_WIDTH + RD) ** (-0.5)
    block_rows = math.gcd(TOKEN_COUNT, 256)
    block_count = TOKEN_COUNT // block_rows

    def attend_block(block_inputs):
        plain_block, turned_block = block_inputs
        scores = (jnp.einsum('qhn,khn->hqk', plain_block, key_plain) + jnp.einsum('qhr,kr->hqk', turned_block, key_turned)) * score_scale
        highest = lax.optimization_barrier(jnp.max(scores, axis=-1, keepdims=True))
        exps = jnp.exp(scores - highest)
        totals = lax.optimization_barrier(jnp.sum(exps, axis=-1))
        weights = lax.optimization_barrier(exps.astype(jnp.bfloat16)).astype(jnp.float32)
        summed = jnp.einsum('hqk,khv->qhv', weights, head_values)
        return (summed / jnp.transpose(totals)[:, :, None]).astype(jnp.bfloat16)
    attended = lax.map(attend_block, (query_plain.reshape(block_count, block_rows, HEAD_COUNT, PLAIN_WIDTH), query_turned.reshape(block_count, block_rows, HEAD_COUNT, RD)))
    attended = attended.reshape(TOKEN_COUNT, HEAD_COUNT * VALUE_WIDTH)
    mixed = jnp.dot(attended, out_weight, preferred_element_type=jnp.float32)
    middle = (resid.astype(jnp.float32) + mixed).astype(jnp.bfloat16)
    normed = rms_scaled(middle, ffn_gain).astype(jnp.bfloat16)
    expert_rows = N_SP * CAP
    flat_ids = expert_ids.reshape(-1).astype(jnp.int32)
    picked = (flat_ids[:, None] == jnp.arange(EXPERTS, dtype=jnp.int32)[None, :]).astype(jnp.int32)
    slot_rank = lax.optimization_barrier(jnp.sum((jnp.cumsum(picked, axis=0) - picked) * picked, axis=1)).astype(jnp.int32)
    slot_index = flat_ids * expert_rows + slot_rank
    sources = jnp.arange(TOKEN_COUNT * TOP, dtype=jnp.int32) // TOP
    owner_row = jnp.zeros((EXPERTS * expert_rows,), jnp.int32).at[slot_index].set(sources)
    filled = jnp.zeros((EXPERTS * expert_rows,), jnp.bool_).at[slot_index].set(True)

    def run_expert(expert_inputs):
        owners, present, gate_matrix, up_matrix, down_matrix = expert_inputs
        rows_in = jnp.where(present[:, None], normed[owners], jnp.zeros((), jnp.bfloat16))
        gate_act = jnp.dot(rows_in, gate_matrix, preferred_element_type=jnp.float32)
        up_act = jnp.dot(rows_in, up_matrix, preferred_element_type=jnp.float32)
        hidden = (jax.nn.silu(gate_act) * up_act).astype(jnp.bfloat16)
        partials = jnp.einsum('rbf,bfd->brd', hidden.astype(jnp.float32).reshape(expert_rows, N_TP, FF_E // N_TP), down_matrix.astype(jnp.float32).reshape(N_TP, FF_E // N_TP, D))
        rounded = lax.optimization_barrier(partials.astype(jnp.bfloat16)).astype(jnp.float32)
        return lax.optimization_barrier(jnp.sum(rounded, axis=0)).astype(jnp.bfloat16)
    outputs = lax.map(run_expert, (owner_row.reshape(EXPERTS, expert_rows), filled.reshape(EXPERTS, expert_rows), gate_weight, up_weight, down_weight))
    chosen_rows = outputs.reshape(EXPERTS * expert_rows, D)[slot_index].astype(jnp.float32) * route_weights.reshape(-1)[:, None]
    routed = lax.optimization_barrier(jnp.sum(chosen_rows.reshape(TOKEN_COUNT, TOP, D), axis=1))
    return (middle.astype(jnp.float32) + routed).astype(jnp.bfloat16)
```

```python
import functools

import jax
import jax.numpy as jnp
from jax import lax
from jax.experimental import pallas as pl
from jax.experimental.pallas import tpu as pltpu
from jax.sharding import PartitionSpec as P

PLAIN_WIDTH = 128
VALUE_WIDTH = 128
LANES = 128
MESH = pl.DeviceIdType.MESH

rope_base = 10000.0
norm_eps = 1e-06


def rotary_table(positions, width):
    half_width = width // 2
    inverse = rope_base ** (-jnp.arange(half_width, dtype=jnp.float32) / half_width)
    turned = positions[:, None] * inverse[None, :]
    return (jnp.cos(turned), jnp.sin(turned))


def turn_pairs(vectors, cosines, sines):
    half_width = vectors.shape[-1] // 2
    front_half = vectors[..., :half_width]
    back_half = vectors[..., half_width:]
    return jnp.concatenate(
        [front_half * cosines - back_half * sines, back_half * cosines + front_half * sines],
        axis=-1,
    )


def rms_scaled(matrix, gain):
    floats = matrix.astype(jnp.float32)
    return floats * lax.rsqrt(jnp.mean(floats * floats, axis=-1, keepdims=True) + norm_eps) * gain


def dot(a, b):
    return jnp.dot(a, b, preferred_element_type=jnp.float32)


def dot_nt(a, b):
    return lax.dot_general(a, b, (((1,), (1,)), ((), ())), preferred_element_type=jnp.float32)


def dot_tn(a, b):
    return lax.dot_general(a, b, (((0,), (0,)), ((), ())), preferred_element_type=jnp.float32)


def layer_kernel(
    cfg,
    query_ref,
    own_ref,
    resid_ref,
    gain_ref,
    ids_ref,
    route_ref,
    kv_hbm,
    ow_hbm,
    gate_hbm,
    up_hbm,
    down_hbm,
    out_ref,
    kv_w,
    ow_w,
    gate_w,
    up_w,
    down_w,
    lat_buf,
    att,
    mix_src,
    mix_buf,
    mid_src,
    mid_buf,
    rows_buf,
    hidden,
    pair_src,
    pair_buf,
    keep,
    sum_src,
    sum_buf,
    ret_src,
    ret_buf,
    load_sem,
    lat_sems,
    mid_sems,
    mix_sems,
    pair_sems,
    sum_sems,
    ret_sems,
):
    n_sp, n_tp, cap, tok, latent_width, rd, heads, top = cfg
    n_y = n_tp // 2
    cols = out_ref.shape[1]
    sp = lax.axis_index("sp")
    tp = lax.axis_index("tp")
    y = tp // 2
    core = lax.rem(tp, 2)
    partner = y * 2 + (1 - core)

    def sp_peer(d):
        return lax.rem(sp + d, n_sp)

    def tp_peer(d):
        return lax.rem(tp + d, n_tp)

    def y_peer(d):
        return lax.rem(y + d, n_y)

    def to(s, t):
        return {"sp": s, "tp": t}

    def loads():
        return [
            pltpu.make_async_copy(kv_hbm, kv_w, load_sem.at[0]),
            pltpu.make_async_copy(ow_hbm, ow_w, load_sem.at[1]),
            pltpu.make_async_copy(gate_hbm.at[0], gate_w, load_sem.at[2]),
            pltpu.make_async_copy(up_hbm.at[0], up_w, load_sem.at[3]),
            pltpu.make_async_copy(down_hbm.at[0], down_w, load_sem.at[4]),
        ]

    barrier = pltpu.get_barrier_semaphore()
    for d in range(1, n_sp):
        pl.semaphore_signal(barrier, inc=1, device_id=to(sp_peer(d), tp), device_id_type=MESH)
    for d in range(1, n_tp):
        pl.semaphore_signal(barrier, inc=1, device_id=to(sp, tp_peer(d)), device_id_type=MESH)
    weights = loads()
    for copy in weights:
        copy.start()
    pl.semaphore_wait(barrier, n_sp + n_tp - 2)

    def gather(source, buf, sems):
        a_send, a_recv, b_send, b_recv, c_send, c_recv = sems

        def a_copy(d, slot, s_to):
            return pltpu.make_async_remote_copy(
                src_ref=source(s_to),
                dst_ref=buf.at[slot, tp],
                send_sem=a_send.at[d],
                recv_sem=a_recv.at[slot],
                device_id=to(s_to, tp),
                device_id_type=MESH,
            )

        def b_copy(s, d):
            return pltpu.make_async_remote_copy(
                src_ref=buf.at[s, tp],
                dst_ref=buf.at[s, tp],
                send_sem=b_send.at[s, d],
                recv_sem=b_recv.at[s, y],
                device_id=to(sp, y_peer(d) * 2 + core),
                device_id_type=MESH,
            )

        def b_arrival(s, y_from):
            return pltpu.make_async_remote_copy(
                src_ref=buf.at[s, y_from * 2 + core],
                dst_ref=buf.at[s, y_from * 2 + core],
                send_sem=b_send.at[s, 0],
                recv_sem=b_recv.at[s, y_from],
                device_id=to(sp, partner),
                device_id_type=MESH,
            )

        def c_copy(s, y_of):
            return pltpu.make_async_remote_copy(
                src_ref=buf.at[s, y_of * 2 + core],
                dst_ref=buf.at[s, y_of * 2 + core],
                send_sem=c_send.at[s, y_of],
                recv_sem=c_recv.at[s, y_of],
                device_id=to(sp, partner),
                device_id_type=MESH,
            )

        def c_arrival(s, y_of):
            return pltpu.make_async_remote_copy(
                src_ref=buf.at[s, y_of * 2 + 1 - core],
                dst_ref=buf.at[s, y_of * 2 + 1 - core],
                send_sem=c_send.at[s, y_of],
                recv_sem=c_recv.at[s, y_of],
                device_id=to(sp, partner),
                device_id_type=MESH,
            )

        @pl.loop(1, n_sp)
        def _(d):
            a_copy(d, sp, sp_peer(d)).start()

        @pl.loop(0, n_sp)
        def _(d):
            s = lax.rem(sp + n_sp - d, n_sp)

            @pl.when(d > 0)
            def _():
                a_copy(d, s, sp_peer(d)).wait_recv()

            for step in range(1, n_y):
                b_copy(s, step).start()
            c_copy(s, y).start()

        @pl.loop(0, n_sp)
        def _(d):
            s = lax.rem(sp + n_sp - d, n_sp)
            for step in range(1, n_y):
                b_arrival(s, y_peer(step)).wait_recv()
                c_copy(s, y_peer(step)).start()

        @pl.loop(0, n_sp)
        def _(d):
            s = lax.rem(sp + n_sp - d, n_sp)
            for step in range(n_y):
                c_arrival(s, y_peer(step)).wait_recv()

        def drain():
            @pl.loop(0, n_sp)
            def _(d):
                @pl.when(d > 0)
                def _():
                    a_copy(d, sp, sp_peer(d)).wait_send()

                for step in range(1, n_y):
                    b_copy(d, step).wait_send()
                for step in range(n_y):
                    c_copy(d, y_peer(step)).wait_send()

        return drain

    own_copy = pltpu.make_async_copy(own_ref.at[tp], lat_buf.at[sp, tp], load_sem.at[5])
    own_copy.start()
    own_copy.wait()
    drain_lat = gather(lambda s_to: own_ref.at[tp], lat_buf, lat_sems)

    n_slots = n_sp * cap
    ids = ids_ref[...]
    expert_iota = lax.broadcasted_iota(jnp.int32, (tok, LANES), 1)
    picks = [(ids[:, k : k + 1] == expert_iota).astype(jnp.float32) for k in range(top)]
    picked = functools.reduce(lambda a, b: a + b, picks)
    earlier = (
        lax.broadcasted_iota(jnp.int32, (tok, tok), 0)
        > lax.broadcasted_iota(jnp.int32, (tok, tok), 1)
    ).astype(jnp.bfloat16)
    before = dot(earlier, picked.astype(jnp.bfloat16))
    slot_iota = lax.broadcasted_iota(jnp.int32, (tok, n_slots), 1)
    slots = []
    for k in range(top):
        rank = jnp.sum(before * picks[k], axis=1, keepdims=True).astype(jnp.int32)
        slots.append((slot_iota == ids[:, k : k + 1] * cap + rank).astype(jnp.float32))
    any_slot = functools.reduce(lambda a, b: a + b, slots)

    keys_all = n_sp * tok
    weights[0].wait()
    latents = lat_buf[:, :, :, :latent_width].reshape(keys_all, latent_width)
    turned = lat_buf[:, :, :, latent_width : latent_width + LANES].reshape(keys_all, LANES)
    scale = (PLAIN_WIDTH + rd) ** (-0.5)
    head_width = PLAIN_WIDTH + VALUE_WIDTH
    for h in range(heads):
        head_kv = dot(latents, kv_w[:, h * head_width : (h + 1) * head_width]).astype(jnp.bfloat16)
        query = query_ref[h]
        scores = dot_nt(query[:, :PLAIN_WIDTH], head_kv[:, :PLAIN_WIDTH])
        scores = (scores + dot_nt(query[:, PLAIN_WIDTH:], turned)) * scale
        exps = jnp.exp(scores - jnp.max(scores, axis=-1, keepdims=True))
        totals = jnp.sum(exps, axis=-1, keepdims=True)
        summed = dot(exps.astype(jnp.bfloat16), head_kv[:, PLAIN_WIDTH:])
        att[:, h * VALUE_WIDTH : (h + 1) * VALUE_WIDTH] = (summed / totals).astype(jnp.bfloat16)
    drain_lat()

    weights[1].wait()
    mix_send, mix_recv = mix_sems

    def out_part(t):
        return dot(att[...], ow_w[:, pl.ds(pl.multiple_of(t * cols, LANES), cols)])

    def mix_copy(d, t_from, t_to):
        return pltpu.make_async_remote_copy(
            src_ref=mix_src.at[d],
            dst_ref=mix_buf.at[t_from],
            send_sem=mix_send.at[d],
            recv_sem=mix_recv.at[t_from],
            device_id=to(sp, t_to),
            device_id_type=MESH,
        )

    @pl.loop(1, n_tp)
    def _(d):
        t_to = tp_peer(d)
        mix_src[d] = out_part(t_to).astype(jnp.bfloat16)
        mix_copy(d, tp, t_to).start()

    mixed = out_part(tp)
    for d in range(1, n_tp):
        t_from = tp_peer(d)
        mix_copy(d, t_from, t_from).wait_recv()
        mixed = mixed + mix_buf[t_from].astype(jnp.float32)
    own_cols = pl.ds(pl.multiple_of(tp * cols, LANES), cols)
    middle = (resid_ref[:, own_cols].astype(jnp.float32) + mixed).astype(jnp.bfloat16)

    outgoing = dot_tn(any_slot.astype(jnp.bfloat16), middle)
    for e in range(n_sp):
        mid_src[e] = outgoing[e * cap : (e + 1) * cap].astype(jnp.bfloat16)
    own_rows = pltpu.make_async_copy(mid_src.at[sp], mid_buf.at[sp, tp], load_sem.at[5])
    own_rows.start()
    own_rows.wait()
    drain_mid = gather(lambda s_to: mid_src.at[s_to], mid_buf, mid_sems)

    gain = gain_ref[...]
    normed = []
    for s in range(n_sp):
        whole = [mid_buf[s, t].astype(jnp.float32) for t in range(n_tp)]
        squares = functools.reduce(
            lambda a, b: a + b, [jnp.sum(w * w, axis=-1, keepdims=True) for w in whole]
        )
        inverse = lax.rsqrt(squares / (n_tp * cols) + norm_eps)
        normed.append(
            jnp.concatenate(
                [w * inverse * gain[:, t * cols : (t + 1) * cols] for t, w in enumerate(whole)],
                axis=1,
            )
        )
    rows_buf[...] = jnp.concatenate(normed, axis=0).astype(jnp.bfloat16)

    weights[2].wait()
    weights[3].wait()
    block = min(256, hidden.shape[1])

    @pl.loop(0, hidden.shape[1] // block)
    def _(j):
        here = pl.ds(pl.multiple_of(j * block, LANES), block)
        gate_act = dot(rows_buf[...], gate_w[:, here])
        up_act = dot(rows_buf[...], up_w[:, here])
        hidden[:, here] = (gate_act / (1.0 + jnp.exp(-gate_act)) * up_act).astype(jnp.bfloat16)

    drain_mid()
    for d in range(1, n_tp):
        mix_copy(d, tp, tp_peer(d)).wait_send()

    weights[4].wait()
    pair_send, pair_recv = pair_sems
    sum_send, sum_recv = sum_sems
    ret_send, ret_recv = ret_sems

    def down_part(t):
        return dot(hidden[...], down_w[:, pl.ds(pl.multiple_of(t * cols, LANES), cols)])

    def pair_copy(d):
        return pltpu.make_async_remote_copy(
            src_ref=pair_src.at[d],
            dst_ref=pair_buf.at[d],
            send_sem=pair_send.at[d],
            recv_sem=pair_recv.at[d],
            device_id=to(sp, partner),
            device_id_type=MESH,
        )

    def sum_copy(d, s, y_from, y_to):
        return pltpu.make_async_remote_copy(
            src_ref=sum_src.at[d, s],
            dst_ref=sum_buf.at[y_from, s],
            send_sem=sum_send.at[d, s],
            recv_sem=sum_recv.at[y_from, s],
            device_id=to(sp, y_to * 2 + core),
            device_id_type=MESH,
        )

    @pl.loop(0, n_y)
    def _(i):
        d = n_y - 1 - i
        part = down_part(y_peer(d) * 2 + 1 - core)
        for s in range(n_sp):
            pair_src[d, s] = part[s * cap : (s + 1) * cap].astype(jnp.bfloat16)
        pair_copy(d).start()
        keep[d] = down_part(y_peer(d) * 2 + core)

    @pl.loop(0, n_y - 1)
    def _(i):
        d = n_y - 1 - i
        pair_copy(d).wait_recv()
        for s in range(n_sp):
            sum_src[d, s] = (
                keep[d, s * cap : (s + 1) * cap] + pair_buf[d, s].astype(jnp.float32)
            ).astype(jnp.bfloat16)

        @pl.loop(0, n_sp)
        def _(k):
            sum_copy(d, sp_peer(k), y, y_peer(d)).start()

    pair_copy(0).wait_recv()

    def ret_copy(d, s_from, s_to):
        return pltpu.make_async_remote_copy(
            src_ref=ret_src.at[d],
            dst_ref=ret_buf.at[s_from],
            send_sem=ret_send.at[d],
            recv_sem=ret_recv.at[s_from],
            device_id=to(s_to, tp),
            device_id_type=MESH,
        )

    @pl.loop(0, n_sp)
    def _(i):
        d = lax.rem(i + 1, n_sp)
        s = sp_peer(d)
        total = keep[0, pl.ds(pl.multiple_of(s * cap, 8), cap)]
        total = total + pair_buf[0, s].astype(jnp.float32)
        for step in range(1, n_y):
            y_from = y_peer(step)
            sum_copy(step, s, y_from, y_from).wait_recv()
            total = total + sum_buf[y_from, s].astype(jnp.float32)
        ret_src[d] = total.astype(jnp.bfloat16)

        @pl.when(d > 0)
        def _():
            ret_copy(d, sp, s).start()

    own_back = pltpu.make_async_copy(ret_src.at[0], ret_buf.at[sp], load_sem.at[5])
    own_back.start()
    own_back.wait()

    @pl.loop(1, n_sp)
    def _(d):
        s_from = sp_peer(d)
        ret_copy(d, s_from, s_from).wait_recv()

    back = jnp.concatenate(
        [ret_buf[e].astype(jnp.float32) for e in range(n_sp)], axis=0
    ).astype(jnp.bfloat16)
    route = route_ref[...]
    routed = functools.reduce(
        lambda a, b: a + b,
        [dot(slots[k].astype(jnp.bfloat16), back) * route[:, k : k + 1] for k in range(top)],
    )
    out_ref[...] = (middle.astype(jnp.float32) + routed).astype(jnp.bfloat16)

    @pl.loop(0, n_y)
    def _(d):
        pair_copy(d).wait_send()

        @pl.when(d > 0)
        def _():
            @pl.loop(0, n_sp)
            def _(k):
                sum_copy(d, k, y, y_peer(d)).wait_send()

    @pl.loop(1, n_sp)
    def _(d):
        ret_copy(d, sp, sp_peer(d)).wait_send()


def shards(
    queries,
    latents,
    rope_keys,
    latent_norm_scale,
    key_value_weight,
    out_weight,
    resid,
    ffn_gain,
    expert_ids,
    route_weights,
    gate_weight,
    up_weight,
    down_weight,
):
    tok, heads, _ = queries.shape
    n_sp = lax.axis_size("sp")
    n_tp = lax.axis_size("tp")
    n_y = n_tp // 2
    width = resid.shape[1]
    latent_width = latents.shape[1]
    rd = rope_keys.shape[1]
    top = expert_ids.shape[1]
    cols = width // n_tp
    capacity = (3 * tok * top + 2 * n_sp - 1) // (2 * n_sp)
    cap = -(-capacity // 8) * 8
    ff = gate_weight.shape[2]

    positions = (lax.axis_index("sp") * tok + jnp.arange(tok, dtype=jnp.int32)).astype(jnp.float32)
    cosines, sines = rotary_table(positions, rd)
    lane_pad = LANES - rd
    query_turned = turn_pairs(
        queries[:, :, PLAIN_WIDTH:].astype(jnp.float32), cosines[:, None, :], sines[:, None, :]
    ).astype(jnp.bfloat16)
    query_all = jnp.concatenate(
        [
            queries[:, :, :PLAIN_WIDTH],
            query_turned,
            jnp.zeros((tok, heads, lane_pad), jnp.bfloat16),
        ],
        axis=2,
    ).transpose(1, 0, 2)
    key_turned = turn_pairs(rope_keys.astype(jnp.float32), cosines, sines).astype(jnp.bfloat16)
    own = jnp.concatenate(
        [
            rms_scaled(latents, latent_norm_scale).astype(jnp.bfloat16),
            key_turned,
            jnp.zeros((tok, lane_pad), jnp.bfloat16),
        ],
        axis=1,
    )
    own = own.reshape(n_tp, tok // n_tp, latent_width + LANES)

    vmem = pl.BlockSpec(memory_space=pltpu.VMEM)
    hbm = pl.BlockSpec(memory_space=pl.ANY)
    bf16, f32 = jnp.bfloat16, jnp.float32
    dma = pltpu.SemaphoreType.DMA

    def gather_sems():
        return (
            dma((n_sp,)),
            dma((n_sp,)),
            dma((n_sp, n_y)),
            dma((n_sp, n_y)),
            dma((n_sp, n_y)),
            dma((n_sp, n_y)),
        )

    scratch = [
        pltpu.VMEM((latent_width, heads * (PLAIN_WIDTH + VALUE_WIDTH)), bf16),
        pltpu.VMEM(out_weight.shape, bf16),
        pltpu.VMEM(gate_weight.shape[1:], bf16),
        pltpu.VMEM(up_weight.shape[1:], bf16),
        pltpu.VMEM(down_weight.shape[1:], bf16),
        pltpu.VMEM((n_sp,) + own.shape, bf16),
        pltpu.VMEM((tok, heads * VALUE_WIDTH), bf16),
        pltpu.VMEM((n_tp, tok, cols), bf16),
        pltpu.VMEM((n_tp, tok, cols), bf16),
        pltpu.VMEM((n_sp, cap, cols), bf16),
        pltpu.VMEM((n_sp, n_tp, cap, cols), bf16),
        pltpu.VMEM((n_sp * cap, width), bf16),
        pltpu.VMEM((n_sp * cap, ff), bf16),
        pltpu.VMEM((n_y, n_sp, cap, cols), bf16),
        pltpu.VMEM((n_y, n_sp, cap, cols), bf16),
        pltpu.VMEM((n_y, n_sp * cap, cols), f32),
        pltpu.VMEM((n_y, n_sp, cap, cols), bf16),
        pltpu.VMEM((n_y, n_sp, cap, cols), bf16),
        pltpu.VMEM((n_sp, cap, cols), bf16),
        pltpu.VMEM((n_sp, cap, cols), bf16),
        dma((6,)),
        gather_sems(),
        gather_sems(),
        (dma((n_tp,)), dma((n_tp,))),
        (dma((n_y,)), dma((n_y,))),
        (dma((n_y, n_sp)), dma((n_y, n_sp))),
        (dma((n_sp,)), dma((n_sp,))),
    ]
    cfg = (n_sp, n_tp, cap, tok, latent_width, rd, heads, top)
    return pl.pallas_call(
        functools.partial(layer_kernel, cfg),
        out_shape=jax.ShapeDtypeStruct((tok, cols), bf16),
        in_specs=[vmem] * 6 + [hbm] * 5,
        out_specs=vmem,
        scratch_shapes=scratch,
        compiler_params=pltpu.CompilerParams(
            collective_id=0, has_side_effects=True, vmem_limit_bytes=60 * 1024 * 1024
        ),
        name="layer",
    )(
        query_all,
        own,
        resid,
        ffn_gain.reshape(1, -1),
        expert_ids,
        route_weights,
        key_value_weight.reshape(latent_width, -1),
        out_weight,
        gate_weight,
        up_weight,
        down_weight,
    )


def solution(mesh):
    placed = (
        P("sp", "tp", None),
        P("sp", None),
        P("sp", None),
        P(),
        P(None, "tp", None),
        P("tp", None),
        P("sp", None),
        P(),
        P("sp", None),
        P("sp", None),
        P("sp", None, "tp"),
        P("sp", None, "tp"),
        P("sp", "tp", None),
    )
    return jax.shard_map(
        shards, mesh=mesh, in_specs=placed, out_specs=P("sp", "tp"), check_vma=False
    )
```

```python
import functools

import jax
import jax.numpy as jnp
from jax import lax
from jax.experimental import pallas as pl
from jax.experimental.pallas import tpu as pltpu
from jax.sharding import PartitionSpec as P

PLAIN_WIDTH = 128
VALUE_WIDTH = 128
LANES = 128
MESH = pl.DeviceIdType.MESH

rope_base = 10000.0
norm_eps = 1e-06


def rotary_table(positions, width):
    half_width = width // 2
    lane = jnp.arange(width, dtype=jnp.int32)
    power = (lane % half_width).astype(jnp.float32) / half_width
    turned = positions[:, None] * (rope_base ** (-power))[None, :]
    sign = jnp.where(lane < half_width, -1.0, 1.0).astype(jnp.float32)
    return (jnp.cos(turned), jnp.sin(turned) * sign[None, :])


def turn_pairs(vectors, cosines, signed_sines):
    half_width = vectors.shape[-1] // 2
    swapped = jnp.concatenate([vectors[:, half_width:], vectors[:, :half_width]], axis=1)
    return vectors * cosines + swapped * signed_sines


def as_column(row):
    size = row.shape[1]
    same = lax.broadcasted_iota(jnp.int32, (size, size), 0) == lax.broadcasted_iota(
        jnp.int32, (size, size), 1
    )
    return jnp.sum(jnp.where(same, jnp.broadcast_to(row, (size, size)), 0.0), axis=1, keepdims=True)


def dot(a, b):
    return jnp.dot(a, b, preferred_element_type=jnp.float32)


def dot_nt(a, b):
    return lax.dot_general(a, b, (((1,), (1,)), ((), ())), preferred_element_type=jnp.float32)


def dot_tn(a, b):
    return lax.dot_general(a, b, (((0,), (0,)), ((), ())), preferred_element_type=jnp.float32)


def layer_kernel(
    cfg,
    query_ref,
    latent_ref,
    rope_ref,
    scale_ref,
    cos_ref,
    sin_ref,
    resid_ref,
    gain_ref,
    ids_ref,
    route_ref,
    kv_hbm,
    ow_hbm,
    gate_hbm,
    up_hbm,
    down_hbm,
    out_ref,
    own_ref,
    query_w,
    kv_raw,
    kv_w,
    ow_w,
    gate_w,
    up_w,
    down_w,
    lat_buf,
    att,
    mix_src,
    mix_buf,
    mid_src,
    mid_buf,
    rows_buf,
    hidden,
    pair_src,
    pair_buf,
    keep,
    sum_src,
    sum_buf,
    ret_src,
    ret_buf,
    load_sem,
    lat_sems,
    mid_sems,
    mix_sems,
    pair_sems,
    sum_sems,
    ret_sems,
):
    n_sp, n_tp, cap, tok, latent_width, rd, heads, top = cfg
    n_y = n_tp // 2
    cols = out_ref.shape[1]
    sp = lax.axis_index("sp")
    tp = lax.axis_index("tp")
    y = tp // 2
    core = lax.rem(tp, 2)
    partner = y * 2 + (1 - core)

    def sp_peer(d):
        return lax.rem(sp + d, n_sp)

    def tp_peer(d):
        return lax.rem(tp + d, n_tp)

    def y_peer(d):
        return lax.rem(y + d, n_y)

    def to(s, t):
        return {"sp": s, "tp": t}

    def loads():
        return [
            pltpu.make_async_copy(kv_hbm, kv_raw, load_sem.at[0]),
            pltpu.make_async_copy(ow_hbm, ow_w, load_sem.at[1]),
            pltpu.make_async_copy(gate_hbm.at[0], gate_w, load_sem.at[2]),
            pltpu.make_async_copy(up_hbm.at[0], up_w, load_sem.at[3]),
            pltpu.make_async_copy(down_hbm.at[0], down_w, load_sem.at[4]),
        ]

    barrier = pltpu.get_barrier_semaphore()
    for d in range(1, n_sp):
        pl.semaphore_signal(barrier, inc=1, device_id=to(sp_peer(d), tp), device_id_type=MESH)
    for d in range(1, n_tp):
        pl.semaphore_signal(barrier, inc=1, device_id=to(sp, tp_peer(d)), device_id_type=MESH)
    weights = loads()
    for copy in weights:
        copy.start()

    latent_rows = latent_ref[...].astype(jnp.float32)
    mean_square = jnp.mean(latent_rows * latent_rows, axis=-1, keepdims=True)
    latent_rows = latent_rows * lax.rsqrt(mean_square + norm_eps) * scale_ref[...]
    cosines, signed_sines = cos_ref[...], sin_ref[...]
    key_rows = turn_pairs(rope_ref[...].astype(jnp.float32), cosines, signed_sines)
    piece = tok // n_tp
    for t in range(n_tp):
        here = slice(t * piece, (t + 1) * piece)
        own_ref[t, :, :latent_width] = latent_rows[here].astype(jnp.bfloat16)
        own_ref[t, :, latent_width : latent_width + rd] = key_rows[here].astype(jnp.bfloat16)
        own_ref[t, :, latent_width + rd :] = jnp.zeros((piece, LANES - rd), jnp.bfloat16)
    pl.semaphore_wait(barrier, n_sp + n_tp - 2)

    def gather(source, buf, sems, meanwhile=None):
        a_send, a_recv, b_send, b_recv, c_send, c_recv = sems

        def a_copy(d, slot, s_to):
            return pltpu.make_async_remote_copy(
                src_ref=source(s_to),
                dst_ref=buf.at[slot, tp],
                send_sem=a_send.at[d],
                recv_sem=a_recv.at[slot],
                device_id=to(s_to, tp),
                device_id_type=MESH,
            )

        def b_copy(s, d):
            return pltpu.make_async_remote_copy(
                src_ref=buf.at[s, tp],
                dst_ref=buf.at[s, tp],
                send_sem=b_send.at[s, d],
                recv_sem=b_recv.at[s, y],
                device_id=to(sp, y_peer(d) * 2 + core),
                device_id_type=MESH,
            )

        def b_arrival(s, y_from):
            return pltpu.make_async_remote_copy(
                src_ref=buf.at[s, y_from * 2 + core],
                dst_ref=buf.at[s, y_from * 2 + core],
                send_sem=b_send.at[s, 0],
                recv_sem=b_recv.at[s, y_from],
                device_id=to(sp, partner),
                device_id_type=MESH,
            )

        def c_copy(s, y_of):
            return pltpu.make_async_remote_copy(
                src_ref=buf.at[s, y_of * 2 + core],
                dst_ref=buf.at[s, y_of * 2 + core],
                send_sem=c_send.at[s, y_of],
                recv_sem=c_recv.at[s, y_of],
                device_id=to(sp, partner),
                device_id_type=MESH,
            )

        def c_arrival(s, y_of):
            return pltpu.make_async_remote_copy(
                src_ref=buf.at[s, y_of * 2 + 1 - core],
                dst_ref=buf.at[s, y_of * 2 + 1 - core],
                send_sem=c_send.at[s, y_of],
                recv_sem=c_recv.at[s, y_of],
                device_id=to(sp, partner),
                device_id_type=MESH,
            )

        @pl.loop(1, n_sp)
        def _(d):
            a_copy(d, sp, sp_peer(d)).start()

        if meanwhile is not None:
            meanwhile()

        @pl.loop(0, n_sp)
        def _(d):
            s = lax.rem(sp + n_sp - d, n_sp)

            @pl.when(d > 0)
            def _():
                a_copy(d, s, sp_peer(d)).wait_recv()

            for step in range(1, n_y):
                b_copy(s, step).start()
            c_copy(s, y).start()

        @pl.loop(0, n_sp)
        def _(d):
            s = lax.rem(sp + n_sp - d, n_sp)
            for step in range(1, n_y):
                b_arrival(s, y_peer(step)).wait_recv()
                c_copy(s, y_peer(step)).start()

        @pl.loop(0, n_sp)
        def _(d):
            s = lax.rem(sp + n_sp - d, n_sp)
            for step in range(n_y):
                c_arrival(s, y_peer(step)).wait_recv()

        def drain():
            @pl.loop(0, n_sp)
            def _(d):
                @pl.when(d > 0)
                def _():
                    a_copy(d, sp, sp_peer(d)).wait_send()

                for step in range(1, n_y):
                    b_copy(d, step).wait_send()
                for step in range(n_y):
                    c_copy(d, y_peer(step)).wait_send()

        return drain

    lat_buf[sp, tp] = own_ref[tp]

    head_width = PLAIN_WIDTH + VALUE_WIDTH

    routing = []

    def turn_queries():
        for h in range(heads):
            plain = query_ref[:, h, :PLAIN_WIDTH]
            rotated = query_ref[:, h, PLAIN_WIDTH:].astype(jnp.float32)
            query_w[h, :, :PLAIN_WIDTH] = plain
            query_w[h, :, PLAIN_WIDTH : PLAIN_WIDTH + rd] = turn_pairs(
                rotated, cosines, signed_sines
            ).astype(jnp.bfloat16)
            query_w[h, :, PLAIN_WIDTH + rd :] = jnp.zeros((tok, LANES - rd), jnp.bfloat16)

        weights[0].wait()
        for h in range(heads):
            kv_w[:, h * head_width : (h + 1) * head_width] = kv_raw[:, h, :]
        n_slots = n_sp * cap
        ids = [as_column(ids_ref[k : k + 1, :].astype(jnp.float32)).astype(jnp.int32) for k in range(top)]
        expert_iota = lax.broadcasted_iota(jnp.int32, (tok, LANES), 1)
        picks = [(ids[k] == expert_iota).astype(jnp.float32) for k in range(top)]
        picked = functools.reduce(lambda a, b: a + b, picks)
        earlier = (
            lax.broadcasted_iota(jnp.int32, (tok, tok), 0)
            > lax.broadcasted_iota(jnp.int32, (tok, tok), 1)
        ).astype(jnp.bfloat16)
        before = dot(earlier, picked.astype(jnp.bfloat16))
        slot_iota = lax.broadcasted_iota(jnp.int32, (tok, n_slots), 1)
        slots = []
        for k in range(top):
            rank = jnp.sum(before * picks[k], axis=1, keepdims=True).astype(jnp.int32)
            slots.append((slot_iota == ids[k] * cap + rank).astype(jnp.float32))
        any_slot = functools.reduce(lambda a, b: a + b, slots)
        routing.extend(slots + [any_slot])

    drain_lat = gather(lambda s_to: own_ref.at[tp], lat_buf, lat_sems, turn_queries)

    *slots, any_slot = routing

    keys_all = n_sp * tok
    latents = lat_buf[:, :, :, :latent_width].reshape(keys_all, latent_width)
    turned = lat_buf[:, :, :, latent_width : latent_width + LANES].reshape(keys_all, LANES)
    scale = (PLAIN_WIDTH + rd) ** (-0.5)
    for h in range(heads):
        head_kv = dot(latents, kv_w[:, h * head_width : (h + 1) * head_width]).astype(jnp.bfloat16)
        query = query_w[h]
        scores = dot_nt(query[:, :PLAIN_WIDTH], head_kv[:, :PLAIN_WIDTH])
        scores = (scores + dot_nt(query[:, PLAIN_WIDTH:], turned)) * scale
        exps = jnp.exp(scores - jnp.max(scores, axis=-1, keepdims=True))
        totals = jnp.sum(exps, axis=-1, keepdims=True)
        summed = dot(exps.astype(jnp.bfloat16), head_kv[:, PLAIN_WIDTH:])
        att[:, h * VALUE_WIDTH : (h + 1) * VALUE_WIDTH] = (summed / totals).astype(jnp.bfloat16)
    drain_lat()

    weights[1].wait()
    mix_send, mix_recv = mix_sems

    def out_part(t):
        return dot(att[...], ow_w[:, pl.ds(pl.multiple_of(t * cols, LANES), cols)])

    def mix_copy(d, t_from, t_to):
        return pltpu.make_async_remote_copy(
            src_ref=mix_src.at[d],
            dst_ref=mix_buf.at[t_from],
            send_sem=mix_send.at[d],
            recv_sem=mix_recv.at[t_from],
            device_id=to(sp, t_to),
            device_id_type=MESH,
        )

    @pl.loop(1, n_tp)
    def _(d):
        t_to = tp_peer(d)
        mix_src[d] = out_part(t_to).astype(jnp.bfloat16)
        mix_copy(d, tp, t_to).start()

    mixed = out_part(tp)
    for d in range(1, n_tp):
        t_from = tp_peer(d)
        mix_copy(d, t_from, t_from).wait_recv()
        mixed = mixed + mix_buf[t_from].astype(jnp.float32)
    own_cols = pl.ds(pl.multiple_of(tp * cols, LANES), cols)
    middle = (resid_ref[:, own_cols].astype(jnp.float32) + mixed).astype(jnp.bfloat16)

    outgoing = dot_tn(any_slot.astype(jnp.bfloat16), middle)
    for e in range(n_sp):
        mid_src[e] = outgoing[e * cap : (e + 1) * cap].astype(jnp.bfloat16)
    mid_buf[sp, tp] = mid_src[sp]
    drain_mid = gather(lambda s_to: mid_src.at[s_to], mid_buf, mid_sems)

    gain = gain_ref[...]
    normed = []
    for s in range(n_sp):
        whole = [mid_buf[s, t].astype(jnp.float32) for t in range(n_tp)]
        squares = functools.reduce(
            lambda a, b: a + b, [jnp.sum(w * w, axis=-1, keepdims=True) for w in whole]
        )
        inverse = lax.rsqrt(squares / (n_tp * cols) + norm_eps)
        normed.append(
            jnp.concatenate(
                [w * inverse * gain[:, t * cols : (t + 1) * cols] for t, w in enumerate(whole)],
                axis=1,
            )
        )
    rows_buf[...] = jnp.concatenate(normed, axis=0).astype(jnp.bfloat16)

    weights[2].wait()
    weights[3].wait()
    block = min(256, hidden.shape[1])

    @pl.loop(0, hidden.shape[1] // block)
    def _(j):
        here = pl.ds(pl.multiple_of(j * block, LANES), block)
        gate_act = dot(rows_buf[...], gate_w[:, here])
        up_act = dot(rows_buf[...], up_w[:, here])
        hidden[:, here] = (gate_act / (1.0 + jnp.exp(-gate_act)) * up_act).astype(jnp.bfloat16)

    drain_mid()
    for d in range(1, n_tp):
        mix_copy(d, tp, tp_peer(d)).wait_send()

    weights[4].wait()
    pair_send, pair_recv = pair_sems
    sum_send, sum_recv = sum_sems
    ret_send, ret_recv = ret_sems

    def down_part(t):
        return dot(hidden[...], down_w[:, pl.ds(pl.multiple_of(t * cols, LANES), cols)])

    def pair_copy(d):
        return pltpu.make_async_remote_copy(
            src_ref=pair_src.at[d],
            dst_ref=pair_buf.at[d],
            send_sem=pair_send.at[d],
            recv_sem=pair_recv.at[d],
            device_id=to(sp, partner),
            device_id_type=MESH,
        )

    def sum_copy(d, s, y_from, y_to):
        return pltpu.make_async_remote_copy(
            src_ref=sum_src.at[d, s],
            dst_ref=sum_buf.at[y_from, s],
            send_sem=sum_send.at[d, s],
            recv_sem=sum_recv.at[y_from, s],
            device_id=to(sp, y_to * 2 + core),
            device_id_type=MESH,
        )

    @pl.loop(0, n_y)
    def _(i):
        d = n_y - 1 - i
        part = down_part(y_peer(d) * 2 + 1 - core)
        for s in range(n_sp):
            pair_src[d, s] = part[s * cap : (s + 1) * cap].astype(jnp.bfloat16)
        pair_copy(d).start()
        keep[d] = down_part(y_peer(d) * 2 + core)

    @pl.loop(0, n_y - 1)
    def _(i):
        d = n_y - 1 - i
        pair_copy(d).wait_recv()
        for s in range(n_sp):
            sum_src[d, s] = (
                keep[d, s * cap : (s + 1) * cap] + pair_buf[d, s].astype(jnp.float32)
            ).astype(jnp.bfloat16)

        @pl.loop(0, n_sp)
        def _(k):
            sum_copy(d, sp_peer(lax.rem(k + 1, n_sp)), y, y_peer(d)).start()

    pair_copy(0).wait_recv()

    def ret_copy(d, s_from, s_to):
        return pltpu.make_async_remote_copy(
            src_ref=ret_src.at[d],
            dst_ref=ret_buf.at[s_from],
            send_sem=ret_send.at[d],
            recv_sem=ret_recv.at[s_from],
            device_id=to(s_to, tp),
            device_id_type=MESH,
        )

    @pl.loop(0, n_sp)
    def _(i):
        d = lax.rem(i + 1, n_sp)
        s = sp_peer(d)
        total = keep[0, pl.ds(pl.multiple_of(s * cap, 8), cap)]
        total = total + pair_buf[0, s].astype(jnp.float32)
        for step in range(1, n_y):
            y_from = y_peer(step)
            sum_copy(step, s, y_from, y_from).wait_recv()
            total = total + sum_buf[y_from, s].astype(jnp.float32)
        ret_src[d] = total.astype(jnp.bfloat16)

        @pl.when(d > 0)
        def _():
            ret_copy(d, sp, s).start()

    ret_buf[sp] = ret_src[0]

    @pl.loop(1, n_sp)
    def _(d):
        s_from = sp_peer(d)
        ret_copy(d, s_from, s_from).wait_recv()

    back = jnp.concatenate(
        [ret_buf[e].astype(jnp.float32) for e in range(n_sp)], axis=0
    ).astype(jnp.bfloat16)
    routed = functools.reduce(
        lambda a, b: a + b,
        [dot(slots[k].astype(jnp.bfloat16), back) * as_column(route_ref[k : k + 1, :]) for k in range(top)],
    )
    out_ref[...] = (middle.astype(jnp.float32) + routed).astype(jnp.bfloat16)

    @pl.loop(0, n_y)
    def _(d):
        pair_copy(d).wait_send()

        @pl.when(d > 0)
        def _():
            @pl.loop(0, n_sp)
            def _(k):
                sum_copy(d, k, y, y_peer(d)).wait_send()

    @pl.loop(1, n_sp)
    def _(d):
        ret_copy(d, sp, sp_peer(d)).wait_send()


def shards(
    queries,
    latents,
    rope_keys,
    latent_norm_scale,
    key_value_weight,
    out_weight,
    resid,
    ffn_gain,
    expert_ids,
    route_weights,
    gate_weight,
    up_weight,
    down_weight,
):
    tok, heads, _ = queries.shape
    n_sp = lax.axis_size("sp")
    n_tp = lax.axis_size("tp")
    n_y = n_tp // 2
    width = resid.shape[1]
    latent_width = latents.shape[1]
    rd = rope_keys.shape[1]
    top = expert_ids.shape[1]
    cols = width // n_tp
    capacity = (3 * tok * top + 2 * n_sp - 1) // (2 * n_sp)
    cap = -(-capacity // 8) * 8
    ff = gate_weight.shape[2]

    positions = (lax.axis_index("sp") * tok + jnp.arange(tok, dtype=jnp.int32)).astype(jnp.float32)
    cosines, signed_sines = rotary_table(positions, rd)

    vmem = pl.BlockSpec(memory_space=pltpu.VMEM)
    hbm = pl.BlockSpec(memory_space=pl.ANY)
    bf16, f32 = jnp.bfloat16, jnp.float32
    dma = pltpu.SemaphoreType.DMA

    def gather_sems():
        return (
            dma((n_sp,)),
            dma((n_sp,)),
            dma((n_sp, n_y)),
            dma((n_sp, n_y)),
            dma((n_sp, n_y)),
            dma((n_sp, n_y)),
        )

    own_shape = (n_tp, tok // n_tp, latent_width + LANES)
    scratch = [
        pltpu.VMEM(own_shape, bf16),
        pltpu.VMEM((heads, tok, PLAIN_WIDTH + LANES), bf16),
        pltpu.VMEM((latent_width, heads, PLAIN_WIDTH + VALUE_WIDTH), bf16),
        pltpu.VMEM((latent_width, heads * (PLAIN_WIDTH + VALUE_WIDTH)), bf16),
        pltpu.VMEM(out_weight.shape, bf16),
        pltpu.VMEM(gate_weight.shape[1:], bf16),
        pltpu.VMEM(up_weight.shape[1:], bf16),
        pltpu.VMEM(down_weight.shape[1:], bf16),
        pltpu.VMEM((n_sp,) + own_shape, bf16),
        pltpu.VMEM((tok, heads * VALUE_WIDTH), bf16),
        pltpu.VMEM((n_tp, tok, cols), bf16),
        pltpu.VMEM((n_tp, tok, cols), bf16),
        pltpu.VMEM((n_sp, cap, cols), bf16),
        pltpu.VMEM((n_sp, n_tp, cap, cols), bf16),
        pltpu.VMEM((n_sp * cap, width), bf16),
        pltpu.VMEM((n_sp * cap, ff), bf16),
        pltpu.VMEM((n_y, n_sp, cap, cols), bf16),
        pltpu.VMEM((n_y, n_sp, cap, cols), bf16),
        pltpu.VMEM((n_y, n_sp * cap, cols), f32),
        pltpu.VMEM((n_y, n_sp, cap, cols), bf16),
        pltpu.VMEM((n_y, n_sp, cap, cols), bf16),
        pltpu.VMEM((n_sp, cap, cols), bf16),
        pltpu.VMEM((n_sp, cap, cols), bf16),
        dma((5,)),
        gather_sems(),
        gather_sems(),
        (dma((n_tp,)), dma((n_tp,))),
        (dma((n_y,)), dma((n_y,))),
        (dma((n_y, n_sp)), dma((n_y, n_sp))),
        (dma((n_sp,)), dma((n_sp,))),
    ]
    cfg = (n_sp, n_tp, cap, tok, latent_width, rd, heads, top)
    return pl.pallas_call(
        functools.partial(layer_kernel, cfg),
        out_shape=jax.ShapeDtypeStruct((tok, cols), bf16),
        in_specs=[vmem] * 10 + [hbm] * 5,
        out_specs=vmem,
        scratch_shapes=scratch,
        compiler_params=pltpu.CompilerParams(
            collective_id=0, has_side_effects=True, vmem_limit_bytes=60 * 1024 * 1024
        ),
        name="layer",
    )(
        queries,
        latents,
        rope_keys,
        latent_norm_scale.reshape(1, -1),
        cosines,
        signed_sines,
        resid,
        ffn_gain.reshape(1, -1),
        expert_ids.T,
        route_weights.T,
        key_value_weight,
        out_weight,
        gate_weight,
        up_weight,
        down_weight,
    )


def solution(mesh):
    placed = (
        P("sp", "tp", None),
        P("sp", None),
        P("sp", None),
        P(),
        P(None, "tp", None),
        P("tp", None),
        P("sp", None),
        P(),
        P("sp", None),
        P("sp", None),
        P("sp", None, "tp"),
        P("sp", None, "tp"),
        P("sp", "tp", None),
    )
    return jax.shard_map(
        shards, mesh=mesh, in_specs=placed, out_specs=P("sp", "tp"), check_vma=False
    )
```
